512 devices in a mesh: grp: 2 (over y), dp: 8 (over x), kv: 16 (over z), tp: 2 (over core).
Axes of the slice: x: 8, y: 2, z: 16, core: 2. Of those that a mesh axis runs over, the one named last changes fastest.
The devices are a block of a 8x8x16 slice.
Arguments:
- tokens: bfloat16 [1024, 4, 4096], P(('grp', 'dp'), None, 'kv'), parts along dimension 0, may hold values from -6 to 6
- w_query: bfloat16 [4096, 2048], P('kv', 'tp'), may hold values from -0.09375 to 0.09375
- w_forget: bfloat16 [4096, 2048], P('kv', 'tp'), may hold values from -0.09375 to 0.09375
- w_input: bfloat16 [4096, 2048], P('kv', 'tp'), may hold values from -0.09375 to 0.09375
- w_gate: bfloat16 [4096, 2048], P('kv', 'tp'), may hold values from -0.09375 to 0.09375
- w_out: bfloat16 [2048, 4096], P('tp', 'kv'), may hold values from -0.125 to 0.125
- gain: float32 [4096], replicated, may hold values from 0.1 to 1.9
- head_gain: float32 [2048], replicated, may hold values from 0.1 to 1.9
- lower_bound: float32 [2048], replicated, may hold values from 0.05 to 0.9
- state: float32 [1024, 16, 128, 128], P(('grp', 'dp', 'kv'), 'tp'), parts along dimension 0, may hold values from -2.4 to 2.4
- last_forget: float32 [1024, 4, 2048], P(('grp', 'dp', 'kv'), None, 'tp'), parts along dimension 0, may hold values from 0.3 to 0.99
- last_values: bfloat16 [1024, 4, 2048], P(('grp', 'dp', 'kv'), None, 'tp'), parts along dimension 0, may hold values from -6 to 6
- accepted: int32 [1024], P(('grp', 'dp', 'kv')), parts along dimension 0, may hold values from 0 to 4
Outputs:
- mixed_out: bfloat16 [1024, 4, 4096], P(('grp', 'dp'), None, ('kv', 'tp')), parts along dimension 0
- taken: float32 [1024, 16, 128, 128], P(('grp', 'dp', 'kv'), 'tp'), parts along dimension 0
The draws below stay inside these ranges and needn't reach their ends.
There are 2 independent parts, one for each index of `grp`. The reference program is written for one: setup_inputs(seed, part) draws one part's arguments, and reference() takes and returns one part's arrays. A program takes and returns all parts, laid end to end along the dimension named above; an argument that names none is the same for every part. Nothing has to cross between parts.
All inputs are finite; a program needn't handle non-finite values.
Results may differ from the reference program's by a relative error of at most 0.0071.
Values may be sent and summed in bfloat16 or wider, within the bound.
A program may use at most 64 MiB of HBM per device.

```python
import jax
import jax.numpy as jnp
from jax import lax

D = 4096
HEADS = 16
HEAD = 128
PROPOSALS = 4
SEQS = 512
N_TP = 2


def touch_ends(drawn, rng, least, high):
    longest = drawn.shape.index(max(drawn.shape))
    spots = []
    for shift in (0, 1):
        where = [jax.random.randint(jax.random.fold_in(rng, axis), (), 0, length) for axis, length in enumerate(drawn.shape)]
        where[longest] = (where[longest] + shift) % drawn.shape[longest]
        spots.append(tuple(where))
    return drawn.at[spots[0]].set(least).at[spots[1]].set(high)


def shard_levels(stream_key, extent, pieces, smallest, high):
    level = 1.0
    for dim, blocks in pieces:
        steps = jax.random.uniform(jax.random.fold_in(jax.random.fold_in(stream_key, 6), dim), (blocks,), jnp.float32, smallest / len(pieces), high / len(pieces))
        level = level * jnp.repeat(jnp.exp(steps), extent[dim] // blocks).reshape((-1,) + (1,) * (len(extent) - 1 - dim))
    return level


def bell_draw(key, shape, spread, most, pieces=(), held_as=jnp.bfloat16):
    array = jax.random.normal(key, shape, jnp.float32) * spread
    if len(pieces) > 0:
        array = shard_levels(key, shape, pieces, -0.22, 0.18) * array
    return jnp.clip(array, min=-most, max=most).astype(held_as)


def setup_inputs(seed: int = 0, part: int = 0) -> dict:
    keys = jax.random.split(jax.random.key(seed), 14)
    part_keys = jax.random.split(jax.random.fold_in(keys[13], part), 14)
    return {
        "tokens": bell_draw(part_keys[0], (SEQS, PROPOSALS, D), 1.0, 6.0, ((0, 8), (2, 16))),
        "w_query": bell_draw(keys[1], (D, HEADS * HEAD), D ** -0.5, 0.09375, ((0, 16), (1, 2))),
        "w_forget": bell_draw(keys[2], (D, HEADS * HEAD), D ** -0.5, 0.09375, ((0, 16), (1, 2))),
        "w_input": bell_draw(keys[3], (D, HEADS * HEAD), D ** -0.5, 0.09375, ((0, 16), (1, 2))),
        "w_gate": bell_draw(keys[4], (D, HEADS * HEAD), D ** -0.5, 0.09375, ((0, 16), (1, 2))),
        "w_out": bell_draw(keys[5], (HEADS * HEAD, D), (HEADS * HEAD) ** -0.5, 0.125, ((0, 2), (1, 16))),
        "gain": jnp.clip(1.0 + 0.18 * jax.random.normal(keys[6], (D,), jnp.float32), 0.1, 1.9),
        "head_gain": jnp.clip(1.0 + 0.18 * jax.random.normal(keys[7], (HEADS * HEAD,), jnp.float32), 0.1, 1.9),
        "lower_bound": jnp.clip(jax.random.uniform(keys[8], (HEADS * HEAD,), jnp.float32, 0.05, 0.9), 0.05, 0.9),
        "state": bell_draw(part_keys[9], (SEQS, HEADS, HEAD, HEAD), 0.3, 2.4, ((0, 128), (1, 2)), jnp.float32),
        "last_forget": jnp.clip(0.3 + 0.69 * jax.random.uniform(part_keys[10], (SEQS, PROPOSALS, HEADS * HEAD), jnp.float32) ** shard_levels(part_keys[10], (SEQS, PROPOSALS, HEADS * HEAD), ((0, 128), (2, 2)), -0.2, 0.2), 0.3, 0.99),
        "last_values": bell_draw(part_keys[11], (SEQS, PROPOSALS, HEADS * HEAD), 1.0, 6.0, ((0, 128), (2, 2))),
        "accepted": touch_ends(jax.random.randint(part_keys[12], (SEQS,), 0, PROPOSALS + 1), jax.random.fold_in(part_keys[12], 1), 0, PROPOSALS).astype(jnp.int32),
    }


EPSILON = 1e-05

def reference(tokens, w_query, w_forget, w_input, w_gate, w_out, gain, head_gain, lower_bound, state, last_forget, last_values, accepted):
    seqs, props, width = tokens.shape
    heads = w_query.shape[1] // HEAD
    tokens_f32 = tokens.astype(jnp.float32)
    row_scale = lax.rsqrt(lax.optimization_barrier(jnp.mean(tokens_f32 * tokens_f32, -1)) + EPSILON).reshape(-1, 1)
    scaled = (tokens_f32 * gain).astype(jnp.bfloat16).reshape(-1, width)

    def project(weight):
        product = jnp.dot(scaled, weight, preferred_element_type=jnp.float32) * row_scale
        return product.reshape(seqs, props, heads, HEAD)
    floor_gate = lower_bound.reshape(heads, HEAD)
    forget = floor_gate + (1.0 - floor_gate) * jax.nn.sigmoid(project(w_forget))
    queries = jax.nn.silu(project(w_query)) * HEAD ** (-0.5)
    values_new = project(w_input)
    gate_path = jax.nn.silu(project(w_gate))
    old_forget = last_forget.reshape(seqs, props, heads, HEAD)
    old_values = last_values.astype(jnp.float32).reshape(seqs, props, heads, HEAD)
    taken = state
    for position in range(PROPOSALS):
        advanced = old_forget[:, position, :, :, None] * taken + (1.0 - old_forget[:, position])[..., None] * old_values[:, position, :, None, :]
        taken = jnp.where((position < accepted)[:, None, None, None], advanced, taken)
    carried = taken
    outputs = []
    for position in range(PROPOSALS):
        carried = forget[:, position, :, :, None] * carried + (1.0 - forget[:, position])[..., None] * values_new[:, position, :, None, :]
        outputs.append(jnp.einsum('shk,shkv->shv', queries[:, position], carried, precision=lax.Precision.HIGHEST))
    recurrent = jnp.stack(outputs, 1)
    normed = recurrent * lax.rsqrt(lax.optimization_barrier(jnp.mean(recurrent * recurrent, -1, keepdims=True)) + EPSILON)
    heads_out = (normed * head_gain.reshape(heads, HEAD) * gate_path).astype(jnp.bfloat16).reshape(seqs * props, heads * HEAD)
    head_cols = heads * HEAD // N_TP
    summed = jnp.zeros((seqs * props, width), jnp.float32)
    for group in range(N_TP):
        part = jnp.dot(heads_out[:, group * head_cols:(group + 1) * head_cols], w_out[group * head_cols:(group + 1) * head_cols], preferred_element_type=jnp.float32)
        summed = summed + lax.optimization_barrier(part.astype(jnp.bfloat16)).astype(jnp.float32)
    return (summed.astype(jnp.bfloat16).reshape(seqs, props, width), taken)
```

```python
import functools

import jax
import jax.numpy as jnp
from jax import lax
from jax.experimental import pallas as pl
from jax.experimental.pallas import tpu as pltpu
from jax.sharding import PartitionSpec as P

HEAD = 128
EPSILON = 1e-05
PIECES = 4
RIGHT, LEFT = 0, 1
F32, BF16 = jnp.float32, jnp.bfloat16


def split(value):
    high = value.astype(BF16)
    return high, (value - high.astype(F32)).astype(BF16)


def kernel(
    n,
    tokens,
    w_query,
    w_forget,
    w_input,
    w_gate,
    w_out,
    gain,
    head_gain,
    lower_bound,
    state,
    last_forget,
    last_values,
    accepted,
    mixed,
    taken,
    tok_v,
    w_v,
    wo_v,
    state_v,
    taken_v,
    t_high,
    t_low,
    columns,
    product,
    squares,
    sums_out,
    sums_in,
    sq_out,
    sq_in,
    gathered,
    halves,
    other,
    load_sem,
    w_sem,
    state_sem,
    taken_sem,
    sum_send,
    sum_recv,
    sq_send,
    sq_recv,
    all_send,
    all_recv,
    half_send,
    half_recv,
):
    half_n = n // 2
    me = lax.axis_index("kv")
    core = lax.axis_index("tp")
    seqs, props, feat = tokens.shape
    rows = seqs * props
    own = rows // n
    own_seqs = own // props
    cols = w_query.shape[1]
    heads = cols // HEAD
    wide = cols // PIECES
    per_piece = wide // HEAD
    width = gain.shape[0] * gain.shape[1]
    weights = (w_query, w_forget, w_input, w_gate)

    def at(offset):
        return lax.rem(me + offset + 2 * n, n)

    load_tok = pltpu.make_async_copy(tokens, tok_v, load_sem.at[0])
    load_tok.start()
    w_loads = []
    for p in range(PIECES):
        for x in range(4):
            part = pl.ds(p * wide, wide)
            copy = pltpu.make_async_copy(
                weights[x].at[:, part], w_v.at[x, :, part], w_sem.at[p, x]
            )
            copy.start()
            w_loads.append(copy)
    s_loads = []
    for h in range(heads):
        copy = pltpu.make_async_copy(state.at[:, h], state_v.at[:, h], state_sem.at[h])
        copy.start()
        s_loads.append(copy)
    load_wo = pltpu.make_async_copy(w_out, wo_v, load_sem.at[1])
    load_wo.start()

    barrier = pltpu.get_barrier_semaphore()
    for peer in ({"kv": at(1)}, {"kv": at(-1)}, {"tp": 1 - core}):
        pl.semaphore_signal(
            barrier, inc=1, device_id=peer, device_id_type=pl.DeviceIdType.MESH
        )

    def remote(src, dst, send_sem, recv_sem, peer):
        return pltpu.make_async_remote_copy(
            src_ref=src,
            dst_ref=dst,
            send_sem=send_sem,
            recv_sem=recv_sem,
            device_id=peer,
            device_id_type=pl.DeviceIdType.MESH,
        )

    def sum_copy(way, step, p):
        return remote(
            sums_out.at[way, step - 1, p],
            sums_in.at[way, step - 1, p],
            sum_send.at[way, step - 1, p],
            sum_recv.at[way, step - 1, p],
            {"kv": at(1 if way == RIGHT else -1)},
        )

    def sq_copy(way, step):
        return remote(
            sq_out.at[way, step - 1],
            sq_in.at[way, step - 1],
            sq_send.at[way, step - 1],
            sq_recv.at[way, step - 1],
            {"kv": at(1 if way == RIGHT else -1)},
        )

    def first_way(p):
        return RIGHT if p < PIECES // 2 else LEFT

    load_tok.wait()
    tok = tok_v[...].astype(F32).reshape(rows, feat)
    gain_row = jnp.concatenate(
        [gain[pl.ds(me * (feat // 128) + i, 1), :] for i in range(feat // 128)], axis=1
    )
    scaled = (tok * gain_row).astype(BF16)

    pl.semaphore_wait(barrier, 3)

    def products(p):
        for x in range(4):
            w_loads[p * 4 + x].wait()
            out = jnp.dot(
                scaled, w_v[x, :, p * wide : (p + 1) * wide], preferred_element_type=F32
            )
            product[p, :, :, x * wide : (x + 1) * wide] = out.reshape(n, own, wide)

    def start_sum(way, step, p):
        dist = half_n + 1 - step
        value = product[p, at(dist if way == RIGHT else -dist)]
        fresh = step == 1 or (step == 2 and first_way(p) != way)
        if not fresh:
            sum_copy(way, step - 1, p).wait_recv()
            value = value + sums_in[way, step - 2, p].astype(F32)
        sums_out[way, step - 1, p] = value.astype(BF16)
        sum_copy(way, step, p).start()

    def start_sq(way, step):
        dist = half_n + 1 - step
        value = squares[at(dist if way == RIGHT else -dist)]
        fresh = step == 1 or (step == 2 and way == LEFT)
        if not fresh:
            sq_copy(way, step - 1).wait_recv()
            value = value + sq_in[way, step - 2]
        sq_out[way, step - 1] = value
        sq_copy(way, step).start()

    for p in range(PIECES):
        products(p)
        start_sum(first_way(p), 1, p)

    row_sum = jnp.sum(tok * tok, axis=1, keepdims=True)
    spread = jnp.where(
        lax.rem(lax.broadcasted_iota(jnp.int32, (rows, 128), 0), own)
        == lax.broadcasted_iota(jnp.int32, (rows, 128), 1),
        row_sum,
        0.0,
    )
    squares[...] = jnp.sum(spread.reshape(n, own, 128), axis=1, keepdims=True)
    start_sq(RIGHT, 1)

    row_of = lax.broadcasted_iota(jnp.int32, (own, 1), 0)
    pos = lax.rem(row_of, props)
    seq_of = row_of // props
    limit = jnp.zeros((own, 1), jnp.int32)
    for s in range(own_seqs):
        limit = jnp.where(seq_of == s, accepted[s], limit)

    def prepare():
        old = last_forget[...].reshape(own, cols)
        kept = pos < limit
        factor = jnp.where(kept, old, 1.0)
        after = jnp.ones_like(factor)
        for step in range(1, props):
            shifted = pltpu.roll(factor, own - step, 0)
            after = after * jnp.where(pos < props - step, shifted, 1.0)
        weight = jnp.where(kept, 1.0 - old, 0.0) * after
        decay = factor * after
        pack = 128 // (2 * own)
        for group in range(heads // pack):
            stack = []
            for h in range(group * pack, (group + 1) * pack):
                stack.append(weight[:, h * HEAD : (h + 1) * HEAD])
                stack.append(decay[:, h * HEAD : (h + 1) * HEAD])
            columns[group] = jnp.concatenate(stack, axis=0).T

    def take(h):
        s_loads[h].wait()
        pack = 128 // (2 * own)
        base = (h % pack) * 2 * own
        table = columns[h // pack]
        values = last_values[:, :, h * HEAD : (h + 1) * HEAD].astype(F32)
        for s in range(own_seqs):
            at_decay = base + own + s * props
            total = table[:, at_decay : at_decay + 1] * state_v[s, h]
            for j in range(props):
                at_weight = base + s * props + j
                total = total + table[:, at_weight : at_weight + 1] * values[s, j : j + 1]
            taken_v[s, h] = total
            high, low = split(total)
            t_high[h, s * HEAD : (s + 1) * HEAD, :] = high
            t_low[h, s * HEAD : (s + 1) * HEAD, :] = low
        pltpu.make_async_copy(taken_v.at[:, h], taken.at[:, h], taken_sem.at[h]).start()

    done = 0
    for step in range(2, half_n + 1):
        if step == 2:
            for p in range(PIECES):
                start_sum(1 - first_way(p), 2, p)
            start_sq(LEFT, 2)
            prepare()
            for p in range(PIECES):
                start_sum(first_way(p), 2, p)
            start_sq(RIGHT, 2)
        else:
            for p in range(PIECES):
                start_sum(RIGHT, step, p)
                start_sum(LEFT, step, p)
            start_sq(RIGHT, step)
            start_sq(LEFT, step)
        until = heads * (step - 1) // (half_n - 1)
        for h in range(done, until):
            take(h)
        done = until

    sq_copy(RIGHT, half_n).wait_recv()
    sq_copy(LEFT, half_n).wait_recv()
    square = squares[me] + sq_in[RIGHT, half_n - 1] + sq_in[LEFT, half_n - 1]
    square = jnp.sum(
        jnp.where(
            lax.broadcasted_iota(jnp.int32, (own, 128), 0)
            == lax.broadcasted_iota(jnp.int32, (own, 128), 1),
            square,
            0.0,
        ),
        axis=1,
        keepdims=True,
    )
    row_scale = lax.rsqrt(square / width + EPSILON)

    def all_copy(src_slot, dst_slot, p, offset):
        return remote(
            gathered.at[src_slot, p],
            gathered.at[dst_slot, p],
            all_send.at[dst_slot, p],
            all_recv.at[dst_slot, p],
            {"kv": at(offset)},
        )

    def spread_from(slot, p):
        if slot < half_n:
            for offset in (1, 2):
                if slot + offset <= half_n:
                    all_copy(slot, slot + offset, p, offset).start()
        if slot == 0 or slot > half_n:
            back = (n - slot) % n
            for offset in (1, 2):
                if back + offset < half_n:
                    all_copy(slot, n - back - offset, p, -offset).start()

    def head_out(p, j, fin):
        h = p * per_piece + j
        lanes = [slice(x * wide + j * HEAD, x * wide + (j + 1) * HEAD) for x in range(4)]
        floor_gate = lower_bound[pl.ds(core * heads + h, 1), :]
        gain_head = head_gain[pl.ds(core * heads + h, 1), :]
        query = jax.nn.silu(fin[:, lanes[0]]) * HEAD ** (-0.5)
        forget = floor_gate + (1.0 - floor_gate) * jax.nn.sigmoid(fin[:, lanes[1]])
        key = 1.0 - forget
        value = fin[:, lanes[2]]
        gate = jax.nn.silu(fin[:, lanes[3]])
        recurrent = jnp.sum(query * key, axis=1, keepdims=True) * value
        decay = query
        for lag in range(1, props):
            ok = pos >= lag
            decay = decay * jnp.where(pos >= lag - 1, pltpu.roll(forget, lag - 1, 0), 1.0)
            score = jnp.sum(decay * pltpu.roll(key, lag, 0), axis=1, keepdims=True)
            recurrent = recurrent + jnp.where(ok, score, 0.0) * pltpu.roll(value, lag, 0)
        decay = decay * jnp.where(pos >= props - 1, pltpu.roll(forget, props - 1, 0), 1.0)
        left = jnp.concatenate(
            [jnp.where(seq_of == s, decay, 0.0) for s in range(own_seqs)], axis=1
        )
        high, low = split(left)
        carried = jnp.dot(
            jnp.concatenate([high, low], axis=0), t_high[h], preferred_element_type=F32
        )
        recurrent = (
            recurrent
            + carried[:own]
            + carried[own:]
            + jnp.dot(high, t_low[h], preferred_element_type=F32)
        )
        mean = jnp.mean(recurrent * recurrent, axis=1, keepdims=True)
        return (recurrent * lax.rsqrt(mean + EPSILON) * gain_head * gate).astype(BF16)

    for p in range(PIECES):
        sum_copy(RIGHT, half_n, p).wait_recv()
        sum_copy(LEFT, half_n, p).wait_recv()
        fin = (
            product[p, me]
            + sums_in[RIGHT, half_n - 1, p].astype(F32)
            + sums_in[LEFT, half_n - 1, p].astype(F32)
        ) * row_scale
        for j in range(per_piece):
            gathered[0, p, :, j * HEAD : (j + 1) * HEAD] = head_out(p, j, fin)
        spread_from(0, p)

    relays = []
    for near in range(2, half_n, 2):
        relays += [near, n - near]
    for slot in relays:
        for p in range(PIECES):
            all_copy(0, slot, p, 1).wait_recv()
            spread_from(slot, p)
    for slot in range(1, n):
        if slot not in relays:
            for p in range(PIECES):
                all_copy(0, slot, p, 1).wait_recv()

    load_wo.wait()
    total = jnp.zeros((rows, wo_v.shape[1]), F32)
    for p in range(PIECES):
        total = total + jnp.dot(
            gathered[:, p].reshape(rows, wide),
            wo_v[p * wide : (p + 1) * wide, :],
            preferred_element_type=F32,
        )
    out_cols = wo_v.shape[1] // 2
    for c in range(2):
        halves[c] = total[:, c * out_cols : (c + 1) * out_cols].astype(BF16)
    swap = remote(
        halves.at[1 - core], other, half_send.at[0], half_recv.at[0], {"tp": 1 - core}
    )
    swap.start()
    swap.wait_recv()
    result = (halves[core].astype(F32) + other[...].astype(F32)).astype(BF16)
    result = result.reshape(n, own_seqs, props, out_cols)
    for slot in range(n):
        mixed[pl.ds(at(-slot) * own_seqs, own_seqs)] = result[slot]

    swap.wait_send()
    for h in range(heads):
        pltpu.make_async_copy(taken_v.at[:, h], taken.at[:, h], taken_sem.at[h]).wait()
    for p in range(PIECES):
        for way in (RIGHT, LEFT):
            for step in range(1, half_n + 1):
                if step > 1 or first_way(p) == way:
                    sum_copy(way, step, p).wait_send()
        for slot in range(1, n):
            all_copy(0, slot, p, 1).wait_send()
    for way in (RIGHT, LEFT):
        for step in range(1, half_n + 1):
            if step > 1 or way == RIGHT:
                sq_copy(way, step).wait_send()


def per_device(
    tokens,
    w_query,
    w_forget,
    w_input,
    w_gate,
    w_out,
    gain,
    head_gain,
    lower_bound,
    state,
    last_forget,
    last_values,
    accepted,
):
    n = lax.axis_size("kv")
    half_n = n // 2
    seqs, props, feat = tokens.shape
    rows = seqs * props
    own = rows // n
    cols = w_query.shape[1]
    heads = cols // HEAD
    wide = cols // PIECES
    out_cols = w_out.shape[1]
    any_space = pl.BlockSpec(memory_space=pl.ANY)
    vmem = pl.BlockSpec(memory_space=pltpu.VMEM)
    dma = pltpu.SemaphoreType.DMA
    return pl.pallas_call(
        functools.partial(kernel, n),
        out_shape=(
            jax.ShapeDtypeStruct((seqs, props, out_cols // 2), BF16),
            jax.ShapeDtypeStruct(state.shape, F32),
        ),
        in_specs=[any_space] * 6
        + [vmem] * 3
        + [any_space]
        + [vmem] * 2
        + [pl.BlockSpec(memory_space=pltpu.SMEM)],
        out_specs=(vmem, any_space),
        scratch_shapes=[
            pltpu.VMEM((seqs, props, feat), BF16),
            pltpu.VMEM((4, feat, cols), BF16),
            pltpu.VMEM(w_out.shape, BF16),
            pltpu.VMEM(state.shape, F32),
            pltpu.VMEM(state.shape, F32),
            pltpu.VMEM((heads, own // props * HEAD, HEAD), BF16),
            pltpu.VMEM((heads, own // props * HEAD, HEAD), BF16),
            pltpu.VMEM((heads * 2 * own // 128, 128, 128), F32),
            pltpu.VMEM((PIECES, n, own, 4 * wide), F32),
            pltpu.VMEM((n, 1, 128), F32),
            pltpu.VMEM((2, half_n, PIECES, own, 4 * wide), BF16),
            pltpu.VMEM((2, half_n, PIECES, own, 4 * wide), BF16),
            pltpu.VMEM((2, half_n, 1, 128), F32),
            pltpu.VMEM((2, half_n, 1, 128), F32),
            pltpu.VMEM((n, PIECES, own, wide), BF16),
            pltpu.VMEM((2, rows, out_cols // 2), BF16),
            pltpu.VMEM((rows, out_cols // 2), BF16),
            dma((2,)),
            dma((PIECES, 4)),
            dma((heads,)),
            dma((heads,)),
            dma((2, half_n, PIECES)),
            dma((2, half_n, PIECES)),
            dma((2, half_n)),
            dma((2, half_n)),
            dma((n, PIECES)),
            dma((n, PIECES)),
            dma((1,)),
            dma((1,)),
        ],
        compiler_params=pltpu.CompilerParams(
            collective_id=0, has_side_effects=True, vmem_limit_bytes=67043328
        ),
    )(
        tokens,
        w_query,
        w_forget,
        w_input,
        w_gate,
        w_out,
        gain.reshape(-1, 128),
        head_gain.reshape(-1, 128),
        lower_bound.reshape(-1, 128),
        state,
        last_forget,
        last_values,
        accepted,
    )


def solution(mesh):
    in_specs = (
        P(("grp", "dp"), None, "kv"),
        P("kv", "tp"),
        P("kv", "tp"),
        P("kv", "tp"),
        P("kv", "tp"),
        P("tp", "kv"),
        P(),
        P(),
        P(),
        P(("grp", "dp", "kv"), "tp", None, None),
        P(("grp", "dp", "kv"), None, "tp"),
        P(("grp", "dp", "kv"), None, "tp"),
        P(("grp", "dp", "kv")),
    )
    out_specs = (P(("grp", "dp"), None, ("kv", "tp")), P(("grp", "dp", "kv"), "tp", None, None))
    return jax.shard_map(
        per_device, mesh=mesh, in_specs=in_specs, out_specs=out_specs, check_vma=False
    )
```

```python
import functools

import jax
import jax.numpy as jnp
from jax import lax
from jax.experimental import pallas as pl
from jax.experimental.pallas import tpu as pltpu
from jax.sharding import PartitionSpec as P

HEAD = 128
EPSILON = 1e-05
GROUPS = 4
SUB = 2
PIECES = GROUPS * SUB
RIGHT, LEFT = 0, 1
F32, BF16 = jnp.float32, jnp.bfloat16


def column_order(n):
    passed = [n - s if back else s for s in range(2, n // 2, 2) for back in (0, 1)]
    return [0] + passed + [s for s in range(1, n) if s not in passed]


def split(value):
    high = value.astype(BF16)
    return high, (value - high.astype(F32)).astype(BF16)


def kernel(
    n,
    tokens,
    w_query,
    w_forget,
    w_input,
    w_gate,
    w_out,
    gain_h,
    head_gain_h,
    lower_bound_h,
    state,
    last_forget_h,
    last_values_h,
    accepted_h,
    mixed,
    taken,
    accepted,
    gain,
    head_gain,
    lower_bound,
    last_forget,
    last_values,
    tok_v,
    scaled_v,
    w_v,
    wo_v,
    state_v,
    t_high,
    t_low,
    weight_v,
    decay_v,
    columns,
    product,
    squares,
    sums_out,
    sums_in,
    sq_out,
    sq_in,
    gathered,
    halves,
    other,
    load_sem,
    w_sem,
    sum_send,
    sum_recv,
    sq_send,
    sq_recv,
    all_send,
    all_recv,
    half_send,
    half_recv,
):
    half_n = n // 2
    me = lax.axis_index("kv")
    core = lax.axis_index("tp")
    seqs, props, feat = tokens.shape
    rows = seqs * props
    own = rows // n
    own_seqs = own // props
    cols = w_query.shape[1]
    heads = cols // HEAD
    wide = cols // PIECES
    per_piece = wide // HEAD
    width = gain.shape[0] * gain.shape[1]
    weights = (w_query, w_forget, w_input, w_gate)

    def at(offset):
        return lax.rem(me + offset + 2 * n, n)

    barrier = pltpu.get_barrier_semaphore()
    for peer in ({"kv": at(1)}, {"kv": at(-1)}, {"tp": 1 - core}):
        pl.semaphore_signal(
            barrier, inc=1, device_id=peer, device_id_type=pl.DeviceIdType.MESH
        )

    load_tok = pltpu.make_async_copy(tokens, tok_v, load_sem.at[0])
    load_tok.start()
    small = []
    for i, (src, dst) in enumerate(
        (
            (gain_h, gain),
            (head_gain_h, head_gain),
            (lower_bound_h, lower_bound),
            (last_forget_h, last_forget),
            (last_values_h, last_values),
            (accepted_h, accepted),
        )
    ):
        small.append(pltpu.make_async_copy(src, dst, load_sem.at[2 + i]))
    small[0].start()
    w_loads = []
    for x in range(4):
        copy = pltpu.make_async_copy(weights[x], w_v.at[x], w_sem.at[x])
        copy.start()
        w_loads.append(copy)
    for copy in small[1:]:
        copy.start()
    load_state = pltpu.make_async_copy(state, state_v, load_sem.at[8])
    load_state.start()
    load_wo = pltpu.make_async_copy(w_out, wo_v, load_sem.at[1])
    load_wo.start()

    def remote(src, dst, send_sem, recv_sem, peer):
        return pltpu.make_async_remote_copy(
            src_ref=src,
            dst_ref=dst,
            send_sem=send_sem,
            recv_sem=recv_sem,
            device_id=peer,
            device_id_type=pl.DeviceIdType.MESH,
        )

    def slot_of(way, step, p, pieces):
        if step == 1:
            return 2 * (half_n - 1) * pieces + p
        return (way * (half_n - 1) + step - 2) * pieces + p

    def sum_copy(way, step, p):
        slot = slot_of(way, step, p, PIECES)
        return remote(
            sums_out.at[slot],
            sums_in.at[slot],
            sum_send.at[0],
            sum_recv.at[slot],
            {"kv": at(1 if way == RIGHT else -1)},
        )

    def sq_copy(way, step):
        slot = slot_of(way, step, 0, 1)
        return remote(
            sq_out.at[slot],
            sq_in.at[slot],
            sq_send.at[0],
            sq_recv.at[slot],
            {"kv": at(1 if way == RIGHT else -1)},
        )

    def first_way(p):
        return RIGHT if p % 2 == 0 else LEFT

    load_tok.wait()
    small[0].wait()
    tok = tok_v[...].astype(F32).reshape(rows, feat)
    gain_row = jnp.concatenate(
        [gain[pl.ds(me * (feat // 128) + i, 1), :] for i in range(feat // 128)], axis=1
    )
    scaled_v[...] = (tok * gain_row).astype(BF16)

    with jax.named_scope("k_barrier"):
        pl.semaphore_wait(barrier, 3)

    def products(g):
        out = jnp.dot(
            scaled_v[...],
            jnp.concatenate(
                [w_v[x, :, g * SUB * wide : (g + 1) * SUB * wide] for x in range(4)], axis=1
            ),
            preferred_element_type=F32,
        )
        for x in range(4):
            for j in range(SUB):
                column = (x * SUB + j) * wide
                product[g * SUB + j, :, :, x * wide : (x + 1) * wide] = out[
                    :, column : column + wide
                ].reshape(n, own, wide)

    for copy in w_loads:
        copy.wait()

    def start_sum(way, step, p):
        dist = half_n + 1 - step
        value = product[p, at(dist if way == RIGHT else -dist)]
        fresh = step == 1 or (step == 2 and first_way(p) != way)
        if not fresh:
            sum_copy(way, step - 1, p).wait_recv()
            value = value + sums_in[slot_of(way, step - 1, p, PIECES)].astype(F32)
        sums_out[slot_of(way, step, p, PIECES)] = value.astype(BF16)
        sum_copy(way, step, p).start()

    def start_sq(way, step):
        dist = half_n + 1 - step
        value = squares[at(dist if way == RIGHT else -dist)]
        fresh = step == 1 or (step == 2 and way == LEFT)
        if not fresh:
            sq_copy(way, step - 1).wait_recv()
            value = value + sq_in[slot_of(way, step - 1, 0, 1)]
        sq_out[slot_of(way, step, 0, 1)] = value
        sq_copy(way, step).start()

    for g in range(GROUPS):
        products(g)
        for p in range(g * SUB, (g + 1) * SUB):
            start_sum(first_way(p), 1, p)
            start_sum(1 - first_way(p), 2, p)

    row_sum = jnp.sum(tok * tok, axis=1, keepdims=True)
    spread = jnp.where(
        lax.rem(lax.broadcasted_iota(jnp.int32, (rows, 128), 0), own)
        == lax.broadcasted_iota(jnp.int32, (rows, 128), 1),
        row_sum,
        0.0,
    )
    squares[...] = jnp.sum(spread.reshape(n, own, 128), axis=1, keepdims=True)
    start_sq(RIGHT, 1)

    row_of = lax.broadcasted_iota(jnp.int32, (own, 1), 0)
    pos = lax.rem(row_of, props)
    seq_of = row_of // props
    def prepare():
        for copy in small[1:]:
            copy.wait()
        limit = jnp.zeros((own, 1), jnp.int32)
        for s in range(own_seqs):
            limit = jnp.where(seq_of == s, accepted[s], limit)
        old = last_forget[...].reshape(own, cols)
        kept = pos < limit
        factor = jnp.where(kept, old, 1.0)
        after = jnp.ones_like(factor)
        for step in range(1, props):
            shifted = pltpu.roll(factor, own - step, 0)
            after = after * jnp.where(pos < props - step, shifted, 1.0)
        weight = jnp.where(kept, 1.0 - old, 0.0) * after
        decay = factor * after
        for h in range(heads):
            lanes = slice(h * HEAD, (h + 1) * HEAD)
            weight_v[h] = weight[:, lanes]
            decay_v[h * own : (h + 1) * own, :] = decay[:, lanes]
        columns[...] = decay_v[...].T
        load_state.wait()

    def blocks(value):
        return jnp.concatenate(
            [jnp.where(seq_of == s, value, 0.0) for s in range(own_seqs)], axis=1
        )

    def take(h):
        weight = blocks(weight_v[h])
        high = weight.astype(BF16)
        rest = weight - high.astype(F32)
        middle = rest.astype(BF16)
        low = (rest - middle.astype(F32)).astype(BF16)
        values = last_values[:, :, h * HEAD : (h + 1) * HEAD].astype(F32)
        values = values.reshape(own, HEAD).astype(BF16)
        added = lax.dot_general(
            jnp.concatenate([high, middle, low], axis=0),
            jnp.concatenate([values] * 3, axis=0),
            (((0,), (0,)), ((), ())),
            preferred_element_type=F32,
        )
        for s in range(own_seqs):
            column = h * own + s * props
            total = (
                columns[:, column : column + 1] * state_v[s, h]
                + added[s * HEAD : (s + 1) * HEAD]
            )
            taken[s, h] = total
            high, low = split(total)
            t_high[h, s * HEAD : (s + 1) * HEAD, :] = high
            t_low[h, s * HEAD : (s + 1) * HEAD, :] = low

    take_after = [1, 1, 1] + [4, 6] + [half_n] * heads
    take_after = take_after[:heads]
    prepare()
    for step in range(1, half_n + 1):
        if step > 1:
            start_sq(RIGHT, step)
            start_sq(LEFT, step)
            for p in range(PIECES):
                for way in (RIGHT, LEFT):
                    if step > 2 or first_way(p) == way:
                        start_sum(way, step, p)
        for h in range(heads):
            if min(take_after[h], half_n) == step:
                take(h)

    sq_copy(RIGHT, half_n).wait_recv()
    sq_copy(LEFT, half_n).wait_recv()
    square = squares[me]
    for way in (RIGHT, LEFT):
        square = square + sq_in[slot_of(way, half_n, 0, 1)]
    square = jnp.sum(
        jnp.where(
            lax.broadcasted_iota(jnp.int32, (own, 128), 0)
            == lax.broadcasted_iota(jnp.int32, (own, 128), 1),
            square,
            0.0,
        ),
        axis=1,
        keepdims=True,
    )
    row_scale = lax.rsqrt(square / width + EPSILON)

    order = column_order(n)
    place = {slot: i for i, slot in enumerate(order)}
    n_passed = 2 * len(range(2, half_n, 2))

    def all_copy(src_slot, dst_slot, p, offset):
        there = place[dst_slot]
        index = (there - 1) * GROUPS + p if there <= n_passed else n_passed * GROUPS
        return remote(
            gathered.at[place[src_slot], p],
            gathered.at[there, p],
            all_send.at[0],
            all_recv.at[index],
            {"kv": at(offset)},
        )

    def spread_from(slot, p):
        if slot < half_n:
            for offset in (1, 2):
                if slot + offset <= half_n:
                    all_copy(slot, slot + offset, p, offset).start()
        if slot == 0 or slot > half_n:
            back = (n - slot) % n
            for offset in (1, 2):
                if back + offset < half_n:
                    all_copy(slot, n - back - offset, p, -offset).start()

    def head_out(p, j, fin):
        h = p * per_piece + j
        lanes = [slice(x * wide + j * HEAD, x * wide + (j + 1) * HEAD) for x in range(4)]
        floor_gate = lower_bound[pl.ds(core * heads + h, 1), :]
        gain_head = head_gain[pl.ds(core * heads + h, 1), :]
        query = jax.nn.silu(fin[:, lanes[0]]) * HEAD ** (-0.5)
        forget = floor_gate + (1.0 - floor_gate) * jax.nn.sigmoid(fin[:, lanes[1]])
        key = 1.0 - forget
        value = fin[:, lanes[2]]
        gate = jax.nn.silu(fin[:, lanes[3]])
        recurrent = jnp.sum(query * key, axis=1, keepdims=True) * value
        decay = query
        for lag in range(1, props):
            ok = pos >= lag
            decay = decay * jnp.where(pos >= lag - 1, pltpu.roll(forget, lag - 1, 0), 1.0)
            score = jnp.sum(decay * pltpu.roll(key, lag, 0), axis=1, keepdims=True)
            recurrent = recurrent + jnp.where(ok, score, 0.0) * pltpu.roll(value, lag, 0)
        decay = decay * jnp.where(pos >= props - 1, pltpu.roll(forget, props - 1, 0), 1.0)
        high, low = split(blocks(decay))
        carried = jnp.dot(
            jnp.concatenate([high, low], axis=0), t_high[h], preferred_element_type=F32
        )
        recurrent = (
            recurrent
            + carried[:own]
            + carried[own:]
            + jnp.dot(high, t_low[h], preferred_element_type=F32)
        )
        mean = jnp.mean(recurrent * recurrent, axis=1, keepdims=True)
        return (recurrent * lax.rsqrt(mean + EPSILON) * gain_head * gate).astype(BF16)

    for p in range(PIECES):
        sum_copy(RIGHT, half_n, p).wait_recv()
        sum_copy(LEFT, half_n, p).wait_recv()
        fin = (
            product[p, me]
            + sums_in[slot_of(RIGHT, half_n, p, PIECES)].astype(F32)
            + sums_in[slot_of(LEFT, half_n, p, PIECES)].astype(F32)
        ) * row_scale
        for j in range(per_piece):
            column = (p % SUB * per_piece + j) * HEAD
            gathered[0, p // SUB, :, column : column + HEAD] = head_out(p, j, fin)
        if p % SUB == SUB - 1:
            spread_from(0, p // SUB)

    for slot in order[1 : 1 + n_passed]:
        for p in range(GROUPS):
            all_copy(0, slot, p, 1).wait_recv()
            spread_from(slot, p)
    ends = gathered.at[pl.ds(1 + n_passed, n - 1 - n_passed)]
    remote(
        ends, ends, all_send.at[0], all_recv.at[n_passed * GROUPS], {"kv": at(1)}
    ).wait_recv()

    load_wo.wait()
    total = jnp.zeros((rows, wo_v.shape[1]), F32)
    for g in range(GROUPS):
        total = total + jnp.dot(
            gathered[:, g].reshape(rows, SUB * wide),
            wo_v[g * SUB * wide : (g + 1) * SUB * wide, :],
            preferred_element_type=F32,
        )
    out_cols = wo_v.shape[1] // 2
    for c in range(2):
        halves[c] = total[:, c * out_cols : (c + 1) * out_cols].astype(BF16)
    swap = remote(
        halves.at[1 - core], other, half_send.at[0], half_recv.at[0], {"tp": 1 - core}
    )
    swap.start()
    swap.wait_recv()
    result = (halves[core].astype(F32) + other[...].astype(F32)).astype(BF16)
    for slot in range(n):
        mixed[pl.ds(at(-order[slot]) * own, own), :] = result[slot * own : (slot + 1) * own]

    swap.wait_send()
    sent = gathered.at[pl.ds(1, n - 1)]
    remote(sent, sent, all_send.at[0], all_recv.at[0], {"kv": at(1)}).wait_send()
    remote(sums_out, sums_in, sum_send.at[0], sum_recv.at[0], {"kv": at(1)}).wait_send()
    remote(sq_out, sq_in, sq_send.at[0], sq_recv.at[0], {"kv": at(1)}).wait_send()


def per_device(
    tokens,
    w_query,
    w_forget,
    w_input,
    w_gate,
    w_out,
    gain,
    head_gain,
    lower_bound,
    state,
    last_forget,
    last_values,
    accepted,
):
    n = lax.axis_size("kv")
    half_n = n // 2
    seqs, props, feat = tokens.shape
    rows = seqs * props
    own = rows // n
    cols = w_query.shape[1]
    heads = cols // HEAD
    wide = cols // PIECES
    out_cols = w_out.shape[1]
    any_space = pl.BlockSpec(memory_space=pltpu.HBM)
    vmem = pl.BlockSpec(memory_space=pltpu.VMEM)
    dma = pltpu.SemaphoreType.DMA
    inputs = [
        tokens,
        w_query,
        w_forget,
        w_input,
        w_gate,
        w_out,
        gain.reshape(-1, 128),
        head_gain.reshape(-1, 128),
        lower_bound.reshape(-1, 128),
        state,
        last_forget,
        last_values,
        accepted,
    ]
    inputs = [pltpu.with_memory_space_constraint(x, pltpu.HBM) for x in inputs]
    mixed, taken = pl.pallas_call(
        functools.partial(kernel, n),
        out_shape=(
            pltpu.VMEM((rows, out_cols // 2), BF16),
            pltpu.VMEM(state.shape, F32),
        ),
        in_specs=[any_space] * 13,
        out_specs=(vmem, vmem),
        scratch_shapes=[
            pltpu.SMEM(accepted.shape, jnp.int32),
            pltpu.VMEM((gain.size // 128, 128), F32),
            pltpu.VMEM((head_gain.size // 128, 128), F32),
            pltpu.VMEM((lower_bound.size // 128, 128), F32),
            pltpu.VMEM(last_forget.shape, F32),
            pltpu.VMEM(last_values.shape, BF16),
            pltpu.VMEM((seqs, props, feat), BF16),
            pltpu.VMEM((rows, feat), BF16),
            pltpu.VMEM((4, feat, cols), BF16),
            pltpu.VMEM(w_out.shape, BF16),
            pltpu.VMEM(state.shape, F32),
            pltpu.VMEM((heads, own // props * HEAD, HEAD), BF16),
            pltpu.VMEM((heads, own // props * HEAD, HEAD), BF16),
            pltpu.VMEM((heads, own, HEAD), F32),
            pltpu.VMEM((heads * own, HEAD), F32),
            pltpu.VMEM((HEAD, heads * own), F32),
            pltpu.VMEM((PIECES, n, own, 4 * wide), F32),
            pltpu.VMEM((n, 1, 128), F32),
            pltpu.VMEM(((n - 1) * PIECES, own, 4 * wide), BF16),
            pltpu.VMEM(((n - 1) * PIECES, own, 4 * wide), BF16),
            pltpu.VMEM((n - 1, 1, 128), F32),
            pltpu.VMEM((n - 1, 1, 128), F32),
            pltpu.VMEM((n, GROUPS, own, SUB * wide), BF16),
            pltpu.VMEM((2, rows, out_cols // 2), BF16),
            pltpu.VMEM((rows, out_cols // 2), BF16),
            dma((9,)),
            dma((4,)),
            dma((1,)),
            dma(((n - 1) * PIECES,)),
            dma((1,)),
            dma((n - 1,)),
            dma((1,)),
            dma(((len(range(2, half_n, 2)) * 2) * GROUPS + 1,)),
            dma((1,)),
            dma((1,)),
        ],
        compiler_params=pltpu.CompilerParams(
            collective_id=0, has_side_effects=True, vmem_limit_bytes=32 * 1024 * 1024
        ),
    )(*inputs)
    return mixed.reshape(seqs, props, out_cols // 2), taken


def solution(mesh):
    in_specs = (
        P(("grp", "dp"), None, "kv"),
        P("kv", "tp"),
        P("kv", "tp"),
        P("kv", "tp"),
        P("kv", "tp"),
        P("tp", "kv"),
        P(),
        P(),
        P(),
        P(("grp", "dp", "kv"), "tp", None, None),
        P(("grp", "dp", "kv"), None, "tp"),
        P(("grp", "dp", "kv"), None, "tp"),
        P(("grp", "dp", "kv")),
    )
    out_specs = (P(("grp", "dp"), None, ("kv", "tp")), P(("grp", "dp", "kv"), "tp", None, None))
    return jax.shard_map(
        per_device, mesh=mesh, in_specs=in_specs, out_specs=out_specs, check_vma=False
    )
```
